32 devices in a mesh: ep: 4 (over y, x), tp: 8 (over z, core).
Axes of the slice: x: 2, y: 2, z: 4, core: 2. Of those that a mesh axis runs over, the one named last changes fastest.
Arguments:
- query_rows: bfloat16 [512, 2048], P('ep', 'tp'), may hold values from -32 to 32
- key_rows: bfloat16 [512, 2048], P('ep', 'tp'), may hold values from -8 to 8
- value_rows: bfloat16 [512, 2048], P('ep', 'tp'), may hold values from -8 to 8
- query_norm_gain: float32 [64], replicated, may hold values from 0.1 to 1.9
- key_gain: float32 [64], replicated, may hold values from 0.1 to 1.9
- break_offset: float32 [32], P('tp'), may hold values from -12 to 3
- mixer_out_weight: bfloat16 [2048, 2048], P('tp'), may hold values from -0.75 to 0.75
- routed_tokens: bfloat16 [4096, 2048], P(('ep', 'tp')), may hold values from -6 to 6
- expert_gain: float32 [2048], replicated, may hold values from 0.1 to 1.9
- routes: int32 [4096, 2], P(('ep', 'tp')), may hold values from 0 to 3, as said below
- route_scores: float32 [4096, 2], P(('ep', 'tp')), may hold values from -6 to 6
- gate_weight: bfloat16 [4, 2048, 3584], P('ep', None, 'tp'), may hold values from -0.125 to 0.125
- up_weight: bfloat16 [4, 2048, 3584], P('ep', None, 'tp'), may hold values from -0.125 to 0.125
- down_weight: bfloat16 [4, 3584, 2048], P('ep', 'tp'), may hold values from -0.09375 to 0.09375
Outputs:
- attention_output: bfloat16 [512, 2048], P(('ep', 'tp'))
- expert_output: bfloat16 [4096, 2048], P(('ep', 'tp'))
The draws below stay inside these ranges and needn't reach their ends.
Inputs may be any that keep to these rules, and one draw needn't show every extreme that they name: `routes`: each row names 2 different experts. Among the rows of one device no expert is named more than 64 times, and one expert is named exactly 64 times by the rows of every device.
All inputs are finite; a program needn't handle non-finite values.
Results may differ from the reference program's by a relative error of at most 0.018.
Values may be sent and summed in bfloat16 or wider, within the bound.
A program may use at most 128 MiB of HBM per device.

```python
import math
import jax
import jax.numpy as jnp
from jax import lax

D = 2048
HEADS = 32
HEAD_DIM = 64
FFE = 3584
TOP_K = 2
TOK_DEV = 128
SEG = 128
SEQUENCE_TOKENS = 512
ROUTED = 4096
EXPERTS = 4
CAP = 64
N_TP = 8


def head_axes(key):
    sample = jax.random.normal(jax.random.fold_in(key, 101), (HEADS, HEAD_DIM), jnp.float32)
    return sample * lax.rsqrt(jnp.mean(sample * sample, axis=1, keepdims=True))


def draw_query_rows(key, part):
    direction = head_axes(key)
    jitter = jax.random.normal(jax.random.fold_in(key, 1), (SEQUENCE_TOKENS, HEADS, HEAD_DIM), jnp.float32)
    rows_out = jnp.clip(0.5 * jitter + direction[None], -32.0, 32.0)
    return rows_out.reshape(SEQUENCE_TOKENS, HEADS * HEAD_DIM).astype(jnp.bfloat16)


def draw_key_rows(key, part):
    direction = head_axes(key)
    blocks_count = SEQUENCE_TOKENS // SEG
    token_position = jnp.arange(SEQUENCE_TOKENS)
    jitter = jax.random.normal(jax.random.fold_in(key, 3), (SEQUENCE_TOKENS, HEADS, HEAD_DIM), jnp.float32)
    low_end = 0.4
    high_end = 1.6
    factor = jnp.exp(jax.random.uniform(jax.random.fold_in(key, 4), (blocks_count,), jnp.float32, jnp.log(low_end), jnp.log(high_end)))
    spread = jax.random.uniform(jax.random.fold_in(key, 5), (SEQUENCE_TOKENS, HEADS), jnp.float32, 0.6, 1.4)
    toward = -factor[token_position // SEG][:, None] * spread
    micro_batches = jax.random.randint(jax.random.fold_in(key, 6), (4,), 0, SEQUENCE_TOKENS)
    broken_stick = jnp.any(token_position[:, None] == micro_batches[None, :], axis=1)
    toward = jnp.where(broken_stick[:, None], 0.2, toward)
    rows_out = jnp.clip(0.5 * jitter + toward[:, :, None] * direction[None], -8.0, 8.0)
    return rows_out.reshape(SEQUENCE_TOKENS, HEADS * HEAD_DIM).astype(jnp.bfloat16)


def draw_value_rows(key, part):
    blocks_count = SEQUENCE_TOKENS // SEG
    levels = jax.random.uniform(jax.random.fold_in(key, 7), (blocks_count, HEADS * HEAD_DIM), jnp.float32, -1.5, 1.5)
    jitter = jax.random.normal(jax.random.fold_in(key, 8), (SEQUENCE_TOKENS, HEADS * HEAD_DIM), jnp.float32)
    rows_out = jnp.clip(jitter + jnp.repeat(levels, SEG, axis=0), -8.0, 8.0)
    return rows_out.astype(jnp.bfloat16)


def draw_break_offset(key, part):
    quick_share = 0.5
    quick = jax.random.uniform(jax.random.fold_in(key, 9), (HEADS,), jnp.float32) < quick_share
    quick_value = jax.random.uniform(jax.random.fold_in(key, 10), (HEADS,), jnp.float32, 2.0, 3.0)
    slow_value = jax.random.uniform(jax.random.fold_in(key, 11), (HEADS,), jnp.float32, 5.0, 6.0) - jnp.log(SEQUENCE_TOKENS * 1.0)
    return jnp.where(quick, quick_value, slow_value).astype(jnp.float32)


def draw_routes(key, part):
    blocks_count = ROUTED // TOK_DEV

    def one_block(block_key):
        reserve = jnp.tile(jnp.arange(1, EXPERTS, dtype=jnp.int32), CAP)
        reserve = jax.random.permutation(jax.random.fold_in(block_key, 1), reserve)
        remainder = jnp.sort(reserve[:TOK_DEV * TOP_K - CAP])
        ordered = jnp.concatenate([jnp.zeros((CAP,), jnp.int32), remainder])
        paired = ordered.reshape(TOP_K, TOK_DEV).T
        shuffle = jax.random.permutation(jax.random.fold_in(block_key, 2), TOK_DEV)
        labels = jax.random.permutation(jax.random.fold_in(block_key, 3), EXPERTS).astype(jnp.int32)
        return labels[paired[shuffle]]
    block_keys = jax.random.split(jax.random.fold_in(key, 13), blocks_count)
    chosen = jax.vmap(one_block)(block_keys).reshape(ROUTED, TOP_K)
    return chosen.astype(jnp.int32)


def block_scale(rng, extent, shards, low, largest):
    factor_of, own = 1.0, jax.random.fold_in(rng, 6)
    for position, parts in shards:
        heights = jnp.exp(jax.random.uniform(jax.random.fold_in(own, position), (parts,), jnp.float32, low / len(shards), largest / len(shards)))
        factor_of = factor_of * jnp.repeat(heights, extent[position] // parts).reshape([-1 if axis == position else 1 for axis in range(len(extent))])
    return factor_of


def noise(rng, dims, deviation, reach, cuts=(), held_as=jnp.bfloat16):
    values = jax.random.normal(rng, dims, jnp.float32) * deviation
    if len(cuts) > 0:
        values = block_scale(rng, dims, cuts, -0.22, 0.18) * values
    return jnp.clip(values, min=-reach, max=reach).astype(held_as)


def setup_inputs(seed: int = 0) -> dict:
    key_list = jax.random.split(jax.random.key(seed), 15)
    return {
        "query_rows": draw_query_rows(jax.random.fold_in(key_list[14], 71), 0),
        "key_rows": draw_key_rows(jax.random.fold_in(key_list[14], 71), 0),
        "value_rows": draw_value_rows(jax.random.fold_in(key_list[14], 71), 0),
        "query_norm_gain": jnp.clip(1.0 + 0.18 * jax.random.normal(key_list[3], (HEAD_DIM,), jnp.float32), 0.1, 1.9),
        "key_gain": jnp.clip(1.0 + 0.18 * jax.random.normal(key_list[4], (HEAD_DIM,), jnp.float32), 0.1, 1.9),
        "break_offset": draw_break_offset(jax.random.fold_in(key_list[14], 71), 0),
        "mixer_out_weight": noise(key_list[6], (HEADS * HEAD_DIM, D), HEAD_DIM ** -0.5, 0.75, ((0, 8),)),
        "routed_tokens": noise(key_list[7], (ROUTED, D), 1.0, 6.0, ((0, 32),)),
        "expert_gain": jnp.clip(1.0 + 0.18 * jax.random.normal(key_list[8], (D,), jnp.float32), 0.1, 1.9),
        "routes": draw_routes(jax.random.fold_in(key_list[14], 71), 0),
        "route_scores": noise(key_list[10], (ROUTED, TOP_K), 1.5, 6.0, ((0, 32),), jnp.float32),
        "gate_weight": noise(key_list[11], (EXPERTS, D, FFE), D ** -0.5, 0.125, ((0, 4), (2, 8))),
        "up_weight": noise(key_list[12], (EXPERTS, D, FFE), D ** -0.5, 0.125, ((0, 4), (2, 8))),
        "down_weight": noise(key_list[13], (EXPERTS, FFE, D), FFE ** -0.5, 0.09375, ((0, 4), (1, 8))),
    }


EPS = 1e-06

def norm_heads(flat, gain):
    count = flat.shape[0]
    split = flat.astype(jnp.float32).reshape(count, -1, HEAD_DIM)
    scaled = split * lax.rsqrt(lax.optimization_barrier(jnp.mean(split * split, axis=2, keepdims=True)) + EPS)
    return (scaled * gain).astype(jnp.bfloat16)

def attention_part(query_rows, key_rows, value_rows, query_norm_gain, key_gain, break_offset, mixer_out_weight):
    length = query_rows.shape[0]
    query_norm = norm_heads(query_rows, query_norm_gain)
    key_norm = norm_heads(key_rows, key_gain)
    value_heads = value_rows.reshape(length, HEADS, HEAD_DIM)
    block_size = math.gcd(512, length)
    gathered = []
    for block_start in range(0, length, block_size):
        block_end = block_start + block_size
        query_place = block_start + jnp.arange(block_size, dtype=jnp.int32)[:, None]
        key_place = jnp.arange(block_end, dtype=jnp.int32)[None, :]
        before = key_place < query_place

        def one_head(inputs):
            query_head, key_head, value_head, offset_value = inputs
            scores = jnp.dot(query_head, key_head.T, preferred_element_type=jnp.float32) * HEAD_DIM ** (-0.5) + offset_value
            log_rise = jax.nn.log_sigmoid(scores)
            log_fail = jnp.where(before, log_rise - scores, 0.0)
            log_after = lax.cumsum(log_fail, axis=1, reverse=True) - log_fail
            weights = jnp.where(before, jnp.exp(log_rise + log_after), 0.0).astype(jnp.bfloat16)
            return jnp.dot(weights, value_head, preferred_element_type=jnp.float32).astype(jnp.bfloat16)
        heads_out = lax.map(one_head, (jnp.moveaxis(query_norm[block_start:block_end], 1, 0), jnp.moveaxis(key_norm[:block_end], 1, 0), jnp.moveaxis(value_heads[:block_end], 1, 0), break_offset))
        gathered.append(jnp.moveaxis(heads_out, 0, 1).reshape(block_size, HEADS * HEAD_DIM))
    heads_mixed = jnp.concatenate(gathered, axis=0)
    group_width = HEADS * HEAD_DIM // N_TP
    running_sum = jnp.zeros((length, D), jnp.float32)
    for group_index in range(N_TP):
        low_edge = group_index * group_width
        term = jnp.dot(heads_mixed[:, low_edge:low_edge + group_width], mixer_out_weight[low_edge:low_edge + group_width], preferred_element_type=jnp.float32).astype(jnp.bfloat16)
        running_sum = running_sum + term.astype(jnp.float32)
    return running_sum.astype(jnp.bfloat16)

def expert_part(routed_tokens, expert_gain, routes, route_scores, gate_weight, up_weight, down_weight):
    row_count = routed_tokens.shape[0]
    as_float = routed_tokens.astype(jnp.float32)
    normed = (as_float * lax.rsqrt(lax.optimization_barrier(jnp.mean(as_float * as_float, axis=1, keepdims=True)) + EPS) * expert_gain).astype(jnp.bfloat16)
    differences = route_scores[:, None, :] - route_scores[:, :, None]
    route_weight = 1.0 / lax.optimization_barrier(jnp.sum(jnp.exp(differences), axis=2))
    flat_routes = routes.reshape(-1).astype(jnp.int32)
    copy_count = flat_routes.shape[0]
    block_count = row_count // TOK_DEV
    member = (flat_routes[:, None] == jnp.arange(EXPERTS, dtype=jnp.int32)[None, :]).astype(jnp.int32)
    member = member.reshape(block_count, TOK_DEV * TOP_K, EXPERTS)
    ahead = lax.optimization_barrier(jnp.sum((jnp.cumsum(member, axis=1) - member) * member, axis=2)).reshape(-1)
    owner = jnp.arange(copy_count, dtype=jnp.int32) // (TOK_DEV * TOP_K)
    slot_index = (owner * CAP + ahead).astype(jnp.int32)
    sources = jnp.repeat(normed, TOP_K, axis=0)
    room = block_count * CAP
    unit_width = FFE // N_TP

    def single_expert(carry, expert_index):
        chosen = flat_routes == expert_index
        target = jnp.where(chosen, slot_index, room).astype(jnp.int32)
        rows_in = jnp.zeros((room, D), jnp.bfloat16).at[target].set(sources, mode='drop')
        gate_part = jnp.dot(rows_in, gate_weight[expert_index], preferred_element_type=jnp.float32)
        up_part = jnp.dot(rows_in, up_weight[expert_index], preferred_element_type=jnp.float32)
        hidden = (jax.nn.silu(gate_part) * up_part).astype(jnp.bfloat16)
        down_here = down_weight[expert_index]
        running_sum = jnp.zeros((room, D), jnp.float32)
        for unit_index in range(N_TP):
            low_edge = unit_index * unit_width
            term = jnp.dot(hidden[:, low_edge:low_edge + unit_width], down_here[low_edge:low_edge + unit_width], preferred_element_type=jnp.float32).astype(jnp.bfloat16)
            running_sum = running_sum + term.astype(jnp.float32)
        result = running_sum.astype(jnp.bfloat16)
        picked = result[jnp.minimum(target, room - 1)]
        return (jnp.where(chosen[:, None], picked.astype(jnp.float32), carry), None)
    results, _ = lax.scan(single_expert, jnp.zeros((copy_count, D), jnp.float32), jnp.arange(EXPERTS, dtype=jnp.int32))
    results = results.reshape(row_count, TOP_K, D)
    return lax.optimization_barrier(jnp.sum(route_weight[..., None] * results, axis=1)).astype(jnp.bfloat16)

def reference(query_rows, key_rows, value_rows, query_norm_gain, key_gain, break_offset, mixer_out_weight, routed_tokens, expert_gain, routes, route_scores, gate_weight, up_weight, down_weight):
    attention_output = attention_part(query_rows, key_rows, value_rows, query_norm_gain, key_gain, break_offset, mixer_out_weight)
    expert_output = expert_part(routed_tokens, expert_gain, routes, route_scores, gate_weight, up_weight, down_weight)
    return (attention_output, expert_output)
```

```python
import functools

import jax
import jax.numpy as jnp
from jax import lax
from jax.experimental import pallas as pl
from jax.experimental.pallas import tpu as pltpu
from jax.sharding import PartitionSpec as P

HEAD_DIM = 64
TOP_K = 2
EPS = 1e-06
TAGS = 128
MESH = pl.DeviceIdType.MESH
F32, BF16 = jnp.float32, jnp.bfloat16

EARLY_SHARE = 96
A_CHUNKS = 4
B_CHUNKS = 2


def dot(a, b):
    return jnp.dot(a, b, preferred_element_type=F32)


def dot_t(a, b):
    return lax.dot_general(a, b, (((1,), (1,)), ((), ())), preferred_element_type=F32)


def split3(x):
    high = x.astype(BF16)
    rest = x - high.astype(F32)
    mid = rest.astype(BF16)
    low = (rest - mid.astype(F32)).astype(BF16)
    return high, mid, low


def rcopy(src, dst, send, recv, dev):
    return pltpu.make_async_remote_copy(
        src_ref=src, dst_ref=dst, send_sem=send, recv_sem=recv, device_id=dev, device_id_type=MESH
    )


def norm_heads(ref, gain):
    out = []
    for start in range(0, ref.shape[1], HEAD_DIM):
        x = ref[:, start : start + HEAD_DIM].astype(F32)
        x = x * lax.rsqrt(jnp.mean(x * x, axis=1, keepdims=True) + EPS)
        out.append((x * gain).astype(BF16))
    return out


def body(
    experts, levels, count, wide, early,
    query, key, value, query_gain, key_gain, offset, mixer, tokens, expert_gain, routes, scores,
    gate, up, down,
    att_out, exp_out,
    wg, wu, wd, wm, normed, xb, xa, xbs, oa, ob, pa, pb, qb, qa, wh, wl,
    ral, rah, mb, rbl, rbh, fa, acc, kv, hm, hmo, ms, rml, rmh,
    lw_sem, pw_send, pw_recv, hm_sem,
    pa_send, pa_recv, kv_send, kv_recv, pb_send, pb_recv, rb_send, rb_recv, ra_send, ra_recv,
    fb_up, fb_dn, fb_recv, fa_up, fa_dn, fa_recv,
    za_send, za_low, za_high, zb_send, zb_low, zb_high, zm_send, zm_low, zm_high,
):
    E, Z, C = experts, levels, count
    A, B = early, wide - early
    slots = TOP_K * C
    cap = slots // E
    R = slots // A_CHUNKS
    TB = C // B_CHUNKS
    ep = lax.axis_index("ep")
    tp = lax.axis_index("tp")
    z = tp // 2
    core = tp % 2
    partner = (ep, tp + 1 - 2 * core)
    above = (ep, tp + 2)
    below = (ep, tp - 2)
    has_low = z > 0
    has_high = z < Z - 1

    def column(d):
        index, bit = ep, 1
        while bit < E:
            if d & bit:
                index = index + bit * (1 - 2 * ((ep // bit) % 2))
            bit *= 2
        return (index, tp)

    local = [
        pltpu.make_async_copy(src, dst.at[0], lw_sem.at[i])
        for i, (src, dst) in enumerate(((gate, wg), (up, wu), (down, wd), (mixer, wm)))
    ]
    for copy in local:
        copy.start()
    barrier = pltpu.get_barrier_semaphore()
    for d in range(1, E):
        pl.semaphore_signal(barrier, inc=1, device_id=column(d), device_id_type=MESH)
    pl.semaphore_signal(barrier, inc=1, device_id=partner, device_id_type=MESH)

    @pl.when(has_low)
    def _():
        pl.semaphore_signal(barrier, inc=1, device_id=below, device_id_type=MESH)

    @pl.when(has_high)
    def _():
        pl.semaphore_signal(barrier, inc=1, device_id=above, device_id_type=MESH)

    x = tokens[...].astype(F32)
    x = x * lax.rsqrt(jnp.mean(x * x, axis=1, keepdims=True) + EPS) * expert_gain[...]
    normed[...] = x.astype(BF16)
    route = routes[...].astype(F32)
    s0, s1 = scores[:, 0:1], scores[:, 1:2]
    w0 = 1.0 / (1.0 + jnp.exp(s1 - s0))
    w1 = 1.0 / (1.0 + jnp.exp(s0 - s1))
    pieces = [route[:, 0:1], route[:, 1:2]]
    for p0, p1 in zip(split3(w0), split3(w1)):
        pieces += [p0.astype(F32), p1.astype(F32)]
    lane = lax.broadcasted_iota(jnp.int32, (C, TAGS), 1)
    tags = jnp.zeros((C, TAGS), F32)
    for i, piece in enumerate(pieces):
        tags = jnp.where(lane == i, piece, tags)
    xb[z, :, :B] = normed[:, A:]
    xb[z, :, B:] = tags.astype(BF16)

    pl.semaphore_wait(barrier, E + has_low.astype(jnp.int32) + has_high.astype(jnp.int32))

    def fwd_b(l, j, sems, dev):
        s = pl.ds(j * TB, TB)
        return rcopy(xb.at[l, s], xb.at[l, s], sems.at[l, j], fb_recv.at[l, j], dev)

    def fwd_a(l, j, sems, dev):
        s = pl.ds(j * R, R)
        return rcopy(xa.at[l, s], xa.at[l, s], sems.at[l, j], fa_recv.at[l, j], dev)

    def both_ways(make, chunks, up_sems, dn_sems):
        for j in range(chunks):

            @pl.when(has_high)
            def _():
                make(z, j, up_sems, above).start()

            @pl.when(has_low)
            def _():
                make(z, j, dn_sems, below).start()

    both_ways(fwd_b, B_CHUNKS, fb_up, fb_dn)

    row = lax.broadcasted_iota(jnp.int32, (C, C), 0)
    col = lax.broadcasted_iota(jnp.int32, (C, C), 1)
    before = (col < row).astype(F32).astype(BF16)
    later = (row > col).astype(F32).astype(BF16)
    slot = lax.broadcasted_iota(jnp.int32, (C, slots), 1)
    shift = cap.bit_length() - 1
    slot_expert = jnp.bitwise_xor(lax.shift_right_logical(slot, shift), ep).astype(F32)
    slot_rank = jnp.bitwise_and(slot, cap - 1).astype(F32)

    def selection(l, t):
        m0 = t[:, 0:1] == slot_expert
        m1 = t[:, 1:2] == slot_expert
        member = jnp.where(jnp.logical_or(m0, m1), 1.0, 0.0)
        rank = dot(before, member.astype(BF16))
        chosen = jnp.where(rank == slot_rank, member, 0.0)
        v0 = t[:, 2:3] + t[:, 4:5] + t[:, 6:7]
        v1 = t[:, 3:4] + t[:, 5:6] + t[:, 7:8]
        weight = chosen * jnp.where(m0, v0, v1)
        high = weight.astype(BF16)
        wh[l] = high
        wl[l] = (weight - high.astype(F32)).astype(BF16)
        return chosen.T.astype(BF16)

    def plane(src, dst, send, recv, d):
        s = pl.ds(d * cap, cap)
        return rcopy(src.at[s], dst.at[s], send, recv, column(d))

    def rest(src, dst, send, recv):
        s = pl.ds(cap, slots - cap)
        return rcopy(src.at[s], dst.at[s], send, recv, column(1))

    def dispatch_b(l, chosen):
        out = dot(chosen, xb[l, :, :B]).astype(BF16)
        xbs[l, :cap] = out[:cap]
        ob[l, cap:] = out[cap:]
        for d in range(1, E):
            plane(ob.at[l], xbs.at[l], pb_send.at[l], pb_recv.at[l], d).start()

    chosen = selection(z, tags)
    out = dot(chosen, normed[:, :A]).astype(BF16)
    xa[z, :cap] = out[:cap]
    oa[cap:] = out[cap:]
    for d in range(1, E):
        plane(oa, xa.at[z], pa_send, pa_recv, d).start()

    swaps = [
        rcopy(src, dst.at[1], pw_send.at[i], pw_recv.at[i], partner)
        for i, (src, dst) in enumerate(((gate, wg), (up, wu), (down, wd), (mixer, wm)))
    ]
    for swap in swaps:
        swap.start()

    heads = key.shape[1] // HEAD_DIM
    aw = key.shape[1]
    kv[:C, :aw] = jnp.concatenate(norm_heads(key, key_gain[...]), axis=1)
    kv[:C, aw:] = value[...]

    def kv_copy(d):
        return rcopy(kv.at[pl.ds(0, C)], kv.at[pl.ds(d * C, C)], kv_send.at[d], kv_recv.at[d], column(d))

    for d in range(1, E):
        kv_copy(d).start()

    dispatch_b(z, chosen)

    rest(oa, xa.at[z], pa_send, pa_recv).wait_recv()
    both_ways(fwd_a, A_CHUNKS, fa_up, fa_dn)

    def attention():
        for d in range(1, E):
            kv_copy(d).wait_recv()
        length = E * C
        query_norm = norm_heads(query, query_gain[...])
        lane = lax.broadcasted_iota(jnp.int32, (C, length), 1)
        bits = C.bit_length() - 1
        owner = jnp.bitwise_xor(lax.shift_right_logical(lane, bits), ep)
        key_place = owner * C + jnp.bitwise_and(lane, C - 1)
        query_place = ep * C + lax.broadcasted_iota(jnp.int32, (C, length), 0)
        allowed = key_place < query_place
        mixed = []
        for h in range(heads):
            part = slice(h * HEAD_DIM, (h + 1) * HEAD_DIM)
            vpart = slice(aw + h * HEAD_DIM, aw + (h + 1) * HEAD_DIM)
            s = dot_t(query_norm[h], kv[:, part]) * HEAD_DIM ** (-0.5) + offset[h]
            soft = jnp.log1p(jnp.exp(-jnp.abs(s)))
            rise = jnp.minimum(s, 0.0) - soft
            fail = jnp.where(allowed, jnp.minimum(-s, 0.0) - soft, 0.0)
            high, mid, low = split3(fail)
            sums = [
                jnp.sum(fail[:, d * C : (d + 1) * C], axis=1, keepdims=True) for d in range(E)
            ]
            afters = []
            for d in range(E):
                b = slice(d * C, (d + 1) * C)
                after = dot(high[:, b], later) + dot(mid[:, b], later) + dot(low[:, b], later)
                for o in range(E):
                    if o != d:
                        later_block = (column(o)[0] > column(d)[0]).astype(F32)
                        after = after + sums[o] * later_block
                afters.append(after)
            exponent = rise + jnp.concatenate(afters, axis=1)
            weights = jnp.where(allowed, jnp.exp(exponent), 0.0).astype(BF16)
            mixed.append(dot(weights, kv[:, vpart]))
        mixed = jnp.concatenate(mixed, axis=1).astype(BF16).astype(F32)
        rows = C // (2 * Z)
        for i in range(Z):
            for k in range(2):
                hm[i, k] = mixed[(2 * i + k) * rows : (2 * i + k + 1) * rows]

    hm_copy = rcopy(hm.at[:, 1 - core], hmo, hm_sem.at[0], hm_sem.at[1], partner)

    def mixer_terms():
        local[3].wait()
        swaps[3].wait_recv()
        hm_copy.wait_recv()
        rows = C // (2 * Z)
        mine = jnp.concatenate([hm[i, core] for i in range(Z)], axis=0).astype(BF16)
        other = jnp.concatenate([hmo[i] for i in range(Z)], axis=0).astype(BF16)
        terms = dot(mine, wm[0]) + dot(other, wm[1])
        for i in range(Z):
            ms[i] = terms[i * rows : (i + 1) * rows].astype(BF16)

    def expert(l):
        rest(ob.at[l], xbs.at[l], pb_send.at[l], pb_recv.at[l]).wait_recv()
        hidden = []
        for i in range(2):
            g = dot(xa[l], wg[i, :A]) + dot(xbs[l], wg[i, A:])
            u = dot(xa[l], wu[i, :A]) + dot(xbs[l], wu[i, A:])
            hidden.append((g / (1.0 + jnp.exp(-g)) * u).astype(BF16))
        tile = 256
        for start in range(A, wide, tile):
            c = slice(start, start + tile)
            y = (dot(hidden[0], wd[0, :, c]) + dot(hidden[1], wd[1, :, c])).astype(BF16)
            pb[l, :, start - A : start - A + tile] = y
        for d in range(1, E):
            plane(pb.at[l], qb.at[l], rb_send.at[l], rb_recv.at[l], d).start()
        qb[l, :cap] = pb[l, :cap]
        for start in range(0, A, tile):
            c = slice(start, start + tile)
            y = (dot(hidden[0], wd[0, :, c]) + dot(hidden[1], wd[1, :, c])).astype(BF16)
            pa[l, :, c] = y

    def ret_a(l, j, buf, recv, dev):
        s = pl.ds(j * R, R)
        return rcopy(pa.at[l, s], buf.at[l, s], za_send.at[l, j], recv.at[l, j], dev)

    def ret_b(l, j, buf, recv, dev):
        s = pl.ds(j * TB, TB)
        return rcopy(mb.at[l, s], buf.at[l, s], zb_send.at[l, j], recv.at[l, j], dev)

    def ret_m(l, buf, recv, dev):
        return rcopy(ms.at[l], buf.at[l], zm_send.at[l], recv.at[l], dev)

    def mix(l, s):
        return dot(wh[l, s], qb[l]) + dot(wl[l, s], qb[l])

    def returns(l, incoming, bufs, recvs, dev):
        for j in range(A_CHUNKS):
            s = pl.ds(j * R, R)

            @pl.when(incoming)
            def _():
                ret_a(l, j, bufs[0], recvs[0], dev).wait_recv()
                pa[l, s] = (pa[l, s].astype(F32) + bufs[0][l, s].astype(F32)).astype(BF16)

            ret_a(l, j, bufs[0], recvs[0], dev).start()

        @pl.when(incoming)
        def _():
            ret_m(l, bufs[2], recvs[2], dev).wait_recv()
            ms[l] = (ms[l].astype(F32) + bufs[2][l].astype(F32)).astype(BF16)

        ret_m(l, bufs[2], recvs[2], dev).start()
        rest(pb.at[l], qb.at[l], rb_send.at[l], rb_recv.at[l]).wait_recv()
        for j in range(B_CHUNKS):
            s = pl.ds(j * TB, TB)
            acc[...] = mix(l, s)

            @pl.when(incoming)
            def _():
                ret_b(l, j, bufs[1], recvs[1], dev).wait_recv()
                acc[...] = acc[...] + bufs[1][l, s].astype(F32)

            mb[l, s] = acc[...].astype(BF16)
            ret_b(l, j, bufs[1], recvs[1], dev).start()

    low_bufs, low_recvs = (ral, rbl, rml), (za_low, zb_low, zm_low)
    high_bufs, high_recvs = (rah, rbh, rmh), (za_high, zb_high, zm_high)

    def slot_step(t, carry):
        low_level, high_level = z - t, z + t
        low_live = low_level >= 0
        high_live = jnp.logical_and(high_level < Z, t > 0)

        @pl.when(t < Z)
        def _():
            @pl.when(t == 0)
            def _():
                attention()
                hm_copy.start()
                for copy in local[:3]:
                    copy.wait()
                for swap in swaps[:3]:
                    swap.wait_recv()

            @pl.when(t > 0)
            def _():
                def arrive(l, onward, sems, dev):
                    for j in range(B_CHUNKS):
                        fwd_b(l, j, sems, dev).wait_recv()

                        @pl.when(onward)
                        def _():
                            fwd_b(l, j, sems, dev).start()

                    dispatch_b(l, selection(l, xb[l, :, B:].astype(F32)))

                def arrive_a(l, onward, sems, dev):
                    for j in range(A_CHUNKS):
                        fwd_a(l, j, sems, dev).wait_recv()

                        @pl.when(onward)
                        def _():
                            fwd_a(l, j, sems, dev).start()

                @pl.when(low_live)
                def _():
                    arrive(low_level, has_high, fb_up, above)

                @pl.when(high_live)
                def _():
                    arrive(high_level, has_low, fb_dn, below)

                @pl.when(low_live)
                def _():
                    arrive_a(low_level, has_high, fa_up, above)

                @pl.when(high_live)
                def _():
                    arrive_a(high_level, has_low, fa_dn, below)

            def side(i, carry):
                expert(z + (2 * i - 1) * t)
                return carry

            lax.fori_loop(
                1 - low_live.astype(jnp.int32), 1 + high_live.astype(jnp.int32), side, 0
            )

            @pl.when(t == 0)
            def _():
                mixer_terms()

        target = t - z

        @pl.when(jnp.logical_and(target > z, target < Z))
        def _():
            returns(target, has_low, low_bufs, low_recvs, above)

        other = 2 * (Z - 1) - t - z

        @pl.when(jnp.logical_and(other >= 0, other < z))
        def _():
            returns(other, has_high, high_bufs, high_recvs, below)

        return carry

    lax.fori_loop(0, 2 * Z - 1, slot_step, 0)

    for j in range(A_CHUNKS):
        s = pl.ds(j * R, R)

        @pl.when(has_low)
        def _():
            ret_a(z, j, ral, za_low, above).wait_recv()
            pa[z, s] = (pa[z, s].astype(F32) + ral[z, s].astype(F32)).astype(BF16)

        @pl.when(has_high)
        def _():
            ret_a(z, j, rah, za_high, below).wait_recv()
            pa[z, s] = (pa[z, s].astype(F32) + rah[z, s].astype(F32)).astype(BF16)

        fa[s] = pa[z, s]
        if j == 0:
            qa[:cap] = pa[z, :cap]
        for d in range(max(1, j * R // cap), (j + 1) * R // cap):
            plane(fa, qa, ra_send, ra_recv, d).start()

    total = ms[z].astype(F32)
    att_out[...] = total.astype(BF16)

    @pl.when(has_low)
    def _():
        ret_m(z, rml, zm_low, above).wait_recv()
        att_out[...] = (att_out[...].astype(F32) + rml[z].astype(F32)).astype(BF16)

    @pl.when(has_high)
    def _():
        ret_m(z, rmh, zm_high, below).wait_recv()
        att_out[...] = (att_out[...].astype(F32) + rmh[z].astype(F32)).astype(BF16)

    rest(pb.at[z], qb.at[z], rb_send.at[z], rb_recv.at[z]).wait_recv()
    for j in range(B_CHUNKS):
        s = pl.ds(j * TB, TB)
        acc[...] = mix(z, s)

        @pl.when(has_low)
        def _():
            ret_b(z, j, rbl, zb_low, above).wait_recv()
            acc[...] = acc[...] + rbl[z, s].astype(F32)

        @pl.when(has_high)
        def _():
            ret_b(z, j, rbh, zb_high, below).wait_recv()
            acc[...] = acc[...] + rbh[z, s].astype(F32)

        exp_out[s, A:] = acc[...].astype(BF16)

    rest(fa, qa, ra_send, ra_recv).wait_recv()
    exp_out[:, :A] = (dot(wh[z], qa[...]) + dot(wl[z], qa[...])).astype(BF16)

    rest(oa, xa.at[z], pa_send, pa_recv).wait_send()
    rest(fa, qa, ra_send, ra_recv).wait_send()
    hm_copy.wait_send()
    for swap in swaps:
        swap.wait_send()
    for d in range(1, E):
        kv_copy(d).wait_send()

    def drain(l, carry):
        rest(ob.at[l], xbs.at[l], pb_send.at[l], pb_recv.at[l]).wait_send()
        rest(pb.at[l], qb.at[l], rb_send.at[l], rb_recv.at[l]).wait_send()

        @pl.when(jnp.logical_and(l <= z, has_high))
        def _():
            for j in range(B_CHUNKS):
                fwd_b(l, j, fb_up, above).wait_send()
            for j in range(A_CHUNKS):
                fwd_a(l, j, fa_up, above).wait_send()

        @pl.when(jnp.logical_and(l >= z, has_low))
        def _():
            for j in range(B_CHUNKS):
                fwd_b(l, j, fb_dn, below).wait_send()
            for j in range(A_CHUNKS):
                fwd_a(l, j, fa_dn, below).wait_send()

        @pl.when(l != z)
        def _():
            for j in range(A_CHUNKS):
                ret_a(l, j, ral, za_low, above).wait_send()
            for j in range(B_CHUNKS):
                ret_b(l, j, rbl, zb_low, above).wait_send()
            ret_m(l, rml, zm_low, above).wait_send()

        return carry

    lax.fori_loop(0, Z, drain, 0)


def layer(
    query, key, value, query_gain, key_gain, offset, mixer, tokens, expert_gain, routes, scores,
    gate, up, down,
):
    E = lax.axis_size("ep")
    Z = lax.axis_size("tp") // 2
    C, D = tokens.shape
    H = gate.shape[2]
    aw = key.shape[1]
    A = D * EARLY_SHARE // 256
    A -= A % 256
    B = D - A
    slots = TOP_K * C
    rows = C // (2 * Z)
    dma = lambda *shape: pltpu.SemaphoreType.DMA(shape)
    vmem = pl.BlockSpec(memory_space=pltpu.VMEM)
    smem = pl.BlockSpec(memory_space=pltpu.SMEM)
    hbm = pl.BlockSpec(memory_space=pl.ANY)
    kernel = functools.partial(body, E, Z, C, D, A)
    NA, NB = A_CHUNKS, B_CHUNKS
    return pl.pallas_call(
        kernel,
        name="step",
        out_shape=(
            jax.ShapeDtypeStruct((rows, D), BF16),
            jax.ShapeDtypeStruct((C, D), BF16),
        ),
        in_specs=[vmem, vmem, vmem, vmem, vmem, smem, hbm, vmem, vmem, vmem, vmem, hbm, hbm, hbm],
        out_specs=(vmem, vmem),
        scratch_shapes=[
            pltpu.VMEM((2, D, H), BF16),
            pltpu.VMEM((2, D, H), BF16),
            pltpu.VMEM((2, H, D), BF16),
            pltpu.VMEM((2, aw, D), BF16),
            pltpu.VMEM((C, D), BF16),
            pltpu.VMEM((Z, C, B + TAGS), BF16),
            pltpu.VMEM((Z, slots, A), BF16),
            pltpu.VMEM((Z, slots, B), BF16),
            pltpu.VMEM((slots, A), BF16),
            pltpu.VMEM((Z, slots, B), BF16),
            pltpu.VMEM((Z, slots, A), BF16),
            pltpu.VMEM((Z, slots, B), BF16),
            pltpu.VMEM((Z, slots, B), BF16),
            pltpu.VMEM((slots, A), BF16),
            pltpu.VMEM((Z, C, slots), BF16),
            pltpu.VMEM((Z, C, slots), BF16),
            pltpu.VMEM((Z, slots, A), BF16),
            pltpu.VMEM((Z, slots, A), BF16),
            pltpu.VMEM((Z, C, B), BF16),
            pltpu.VMEM((Z, C, B), BF16),
            pltpu.VMEM((Z, C, B), BF16),
            pltpu.VMEM((slots, A), BF16),
            pltpu.VMEM((C // NB, B), F32),
            pltpu.VMEM((E * C, 2 * aw), BF16),
            pltpu.VMEM((Z, 2, rows, aw), F32),
            pltpu.VMEM((Z, rows, aw), F32),
            pltpu.VMEM((Z, rows, D), BF16),
            pltpu.VMEM((Z, rows, D), BF16),
            pltpu.VMEM((Z, rows, D), BF16),
            dma(4), dma(4), dma(4), dma(2),
            pltpu.SemaphoreType.DMA, pltpu.SemaphoreType.DMA,
            dma(E), dma(E),
            dma(Z), dma(Z),
            dma(Z), dma(Z),
            pltpu.SemaphoreType.DMA, pltpu.SemaphoreType.DMA,
            dma(Z, NB), dma(Z, NB), dma(Z, NB),
            dma(Z, NA), dma(Z, NA), dma(Z, NA),
            dma(Z, NA), dma(Z, NA), dma(Z, NA),
            dma(Z, NB), dma(Z, NB), dma(Z, NB),
            dma(Z), dma(Z), dma(Z),
        ],
        compiler_params=pltpu.CompilerParams(
            collective_id=0, has_side_effects=True, vmem_limit_bytes=62 * 1024 * 1024
        ),
    )(
        query, key, value, query_gain[None], key_gain[None], offset, mixer, tokens,
        expert_gain[None], routes, scores, gate[0], up[0], down[0],
    )


def solution(mesh):
    in_specs = (
        P("ep", "tp"),
        P("ep", "tp"),
        P("ep", "tp"),
        P(),
        P(),
        P("tp"),
        P("tp", None),
        P(("ep", "tp"), None),
        P(),
        P(("ep", "tp"), None),
        P(("ep", "tp"), None),
        P("ep", None, "tp"),
        P("ep", None, "tp"),
        P("ep", "tp", None),
    )
    out_specs = (P(("ep", "tp"), None), P(("ep", "tp"), None))
    return jax.shard_map(layer, mesh=mesh, in_specs=in_specs, out_specs=out_specs, check_vma=False)
```

```python
import functools

import jax
import jax.numpy as jnp
from jax import lax
from jax.experimental import pallas as pl
from jax.experimental.pallas import tpu as pltpu
from jax.sharding import PartitionSpec as P

HEAD_DIM = 64
TOP_K = 2
EPS = 1e-06
TAGS = 128
MESH = pl.DeviceIdType.MESH
F32, BF16 = jnp.float32, jnp.bfloat16

EARLY_SHARE = 96
A_CHUNKS = 4
B_CHUNKS = 2
B_BACK = 4


def dot(a, b):
    return jnp.dot(a, b, preferred_element_type=F32)


def dot_t(a, b):
    return lax.dot_general(a, b, (((1,), (1,)), ((), ())), preferred_element_type=F32)


def split3(x):
    high = x.astype(BF16)
    rest = x - high.astype(F32)
    mid = rest.astype(BF16)
    low = (rest - mid.astype(F32)).astype(BF16)
    return high, mid, low


def rcopy(src, dst, send, recv, dev):
    return pltpu.make_async_remote_copy(
        src_ref=src, dst_ref=dst, send_sem=send, recv_sem=recv, device_id=dev, device_id_type=MESH
    )


def norm_heads(ref, gain):
    out = []
    for start in range(0, ref.shape[1], HEAD_DIM):
        x = ref[:, start : start + HEAD_DIM].astype(F32)
        x = x * lax.rsqrt(jnp.mean(x * x, axis=1, keepdims=True) + EPS)
        out.append((x * gain).astype(BF16))
    return out


def body(
    experts, levels, count, wide, early,
    query, key, value, query_gain, key_gain, offset, mixer, tokens, expert_gain, routes, scores,
    gate, up, down,
    att_out, exp_out,
    wg, wu, wd, wm, normed, xb, xa, xbs, oa, ob, pa, pb, qb, qa, wh, wl,
    ral, rah, mb, rbl, rbh, fa, acc, kv, hm, hmo, ms, rml, rmh,
    lw_sem, pw_send, pw_recv, hm_sem,
    pa_send, pa_recv, kv_send, kv_recv, pb_send, pb_recv, rb_send, rb_recv, ra_send, ra_recv,
    fb_up, fb_dn, fb_recv, fa_up, fa_dn, fa_recv,
    za_send, za_low, za_high, zb_send, zb_low, zb_high, zm_send, zm_low, zm_high,
):
    E, Z, C = experts, levels, count
    A, B = early, wide - early
    slots = TOP_K * C
    cap = slots // E
    R = slots // A_CHUNKS
    TB = C // B_CHUNKS
    TR = C // B_BACK
    ep = lax.axis_index("ep")
    tp = lax.axis_index("tp")
    z = tp // 2
    core = tp % 2
    partner = (ep, tp + 1 - 2 * core)
    above = (ep, tp + 2)
    below = (ep, tp - 2)
    has_low = z > 0
    has_high = z < Z - 1

    def column(d):
        index, bit = ep, 1
        while bit < E:
            if d & bit:
                index = index + bit * (1 - 2 * ((ep // bit) % 2))
            bit *= 2
        return (index, tp)

    local = [
        pltpu.make_async_copy(src, dst.at[0], lw_sem.at[i])
        for i, (src, dst) in enumerate(((gate, wg), (up, wu), (down, wd), (mixer, wm)))
    ]
    for copy in local:
        copy.start()
    barrier = pltpu.get_barrier_semaphore()
    for d in range(1, E):
        pl.semaphore_signal(barrier, inc=1, device_id=column(d), device_id_type=MESH)
    pl.semaphore_signal(barrier, inc=1, device_id=partner, device_id_type=MESH)

    @pl.when(has_low)
    def _():
        pl.semaphore_signal(barrier, inc=1, device_id=below, device_id_type=MESH)

    @pl.when(has_high)
    def _():
        pl.semaphore_signal(barrier, inc=1, device_id=above, device_id_type=MESH)

    x = tokens[...].astype(F32)
    x = x * lax.rsqrt(jnp.mean(x * x, axis=1, keepdims=True) + EPS) * expert_gain[...]
    normed[...] = x.astype(BF16)
    route = routes[...].astype(F32)
    s0, s1 = scores[0:1], scores[1:2]
    w0 = 1.0 / (1.0 + jnp.exp(s1 - s0))
    w1 = 1.0 / (1.0 + jnp.exp(s0 - s1))
    pieces = [route[0:1], route[1:2]]
    for p0, p1 in zip(split3(w0), split3(w1)):
        pieces += [p0.astype(F32), p1.astype(F32)]
    line = lax.broadcasted_iota(jnp.int32, (TAGS, C), 0)
    tags = jnp.zeros((TAGS, C), F32)
    for i, piece in enumerate(pieces):
        tags = jnp.where(line == i, piece, tags)
    tags = tags.T
    xb[z, :, :B] = normed[:, A:]
    xb[z, :, B:] = tags.astype(BF16)

    def fwd_b(l, j, sems, dev):
        s = pl.ds(j * TB, TB)
        return rcopy(xb.at[l, s], xb.at[l, s], sems.at[l, j], fb_recv.at[l, j], dev)

    def fwd_a(l, j, sems, dev):
        s = pl.ds(j * R, R)
        return rcopy(xa.at[l, s], xa.at[l, s], sems.at[l, j], fa_recv.at[l, j], dev)

    def both_ways(make, chunks, up_sems, dn_sems):
        for j in range(chunks):

            @pl.when(has_high)
            def _():
                make(z, j, up_sems, above).start()

            @pl.when(has_low)
            def _():
                make(z, j, dn_sems, below).start()

    row = lax.broadcasted_iota(jnp.int32, (C, C), 0)
    col = lax.broadcasted_iota(jnp.int32, (C, C), 1)
    before = (col < row).astype(F32).astype(BF16)
    later = (row > col).astype(F32).astype(BF16)
    slot = lax.broadcasted_iota(jnp.int32, (C, slots), 1)
    shift = cap.bit_length() - 1
    slot_expert = jnp.bitwise_xor(lax.shift_right_logical(slot, shift), ep).astype(F32)
    slot_rank = jnp.bitwise_and(slot, cap - 1).astype(F32)

    def selection(l, t):
        m0 = t[:, 0:1] == slot_expert
        m1 = t[:, 1:2] == slot_expert
        member = jnp.where(jnp.logical_or(m0, m1), 1.0, 0.0)
        rank = dot(before, member.astype(BF16))
        chosen = jnp.where(rank == slot_rank, member, 0.0)
        v0 = t[:, 2:3] + t[:, 4:5] + t[:, 6:7]
        v1 = t[:, 3:4] + t[:, 5:6] + t[:, 7:8]
        weight = chosen * jnp.where(m0, v0, v1)
        high = weight.astype(BF16)
        wh[l] = high
        wl[l] = (weight - high.astype(F32)).astype(BF16)
        return chosen.T.astype(BF16)

    def plane(src, dst, send, recv, d):
        s = pl.ds(d * cap, cap)
        return rcopy(src.at[s], dst.at[s], send, recv, column(d))

    def rest(src, dst, send, recv):
        s = pl.ds(cap, slots - cap)
        return rcopy(src.at[s], dst.at[s], send, recv, column(1))

    def dispatch_b(l, chosen):
        out = dot(chosen, xb[l, :, :B]).astype(BF16)
        xbs[l, :cap] = out[:cap]
        ob[l, cap:] = out[cap:]
        for d in range(1, E):
            plane(ob.at[l], xbs.at[l], pb_send.at[l], pb_recv.at[l], d).start()

    chosen = selection(z, tags)
    out = dot(chosen, normed[:, :A]).astype(BF16)
    xa[z, :cap] = out[:cap]
    oa[cap:] = out[cap:]
    with jax.named_scope("barrier"):
     pl.semaphore_wait(barrier, E + has_low.astype(jnp.int32) + has_high.astype(jnp.int32))

    both_ways(fwd_b, B_CHUNKS, fb_up, fb_dn)
    for d in range(1, E):
        plane(oa, xa.at[z], pa_send, pa_recv, d).start()

    swaps = [
        rcopy(src, dst.at[1], pw_send.at[i], pw_recv.at[i], partner)
        for i, (src, dst) in enumerate(((gate, wg), (up, wu), (down, wd), (mixer, wm)))
    ]
    for swap in swaps:
        swap.start()

    dispatch_b(z, chosen)

    with jax.named_scope("w_own_a"):
        rest(oa, xa.at[z], pa_send, pa_recv).wait_recv()
    both_ways(fwd_a, A_CHUNKS, fa_up, fa_dn)

    def on_sides(t, work):
        @pl.when(z - t >= 0)
        def _():
            work(z - t, has_high, 0)

        @pl.when(z + t < Z)
        def _():
            work(z + t, has_low, 1)

    def arrive_b(l, onward, side):
        sems, dev = ((fb_up, above), (fb_dn, below))[side]
        for j in range(B_CHUNKS):
            with jax.named_scope("w_fwd_b"):
                fwd_b(l, j, sems, dev).wait_recv()

            @pl.when(onward)
            def _():
                fwd_b(l, j, sems, dev).start()

        with jax.named_scope("dispatch"):
            dispatch_b(l, selection(l, xb[l, :, B:].astype(F32)))

    def arrive_a(l, onward, side):
        sems, dev = ((fa_up, above), (fa_dn, below))[side]
        for j in range(A_CHUNKS):
            with jax.named_scope("w_fwd_a"):
                fwd_a(l, j, sems, dev).wait_recv()

            @pl.when(onward)
            def _():
                fwd_a(l, j, sems, dev).start()

    on_sides(1, arrive_b)

    heads = key.shape[1] // HEAD_DIM
    aw = key.shape[1]
    kv[:C, :aw] = jnp.concatenate(norm_heads(key, key_gain[...]), axis=1)
    kv[:C, aw:] = value[...]

    def kv_copy(d):
        return rcopy(kv.at[pl.ds(0, C)], kv.at[pl.ds(d * C, C)], kv_send.at[d], kv_recv.at[d], column(d))

    for d in range(1, E):
        kv_copy(d).start()

    def attention():
        with jax.named_scope("w_kv"):
         for d in range(1, E):
            kv_copy(d).wait_recv()
        length = E * C
        query_norm = norm_heads(query, query_gain[...])
        lane = lax.broadcasted_iota(jnp.int32, (C, length), 1)
        bits = C.bit_length() - 1
        owner = jnp.bitwise_xor(lax.shift_right_logical(lane, bits), ep)
        key_place = owner * C + jnp.bitwise_and(lane, C - 1)
        query_place = ep * C + lax.broadcasted_iota(jnp.int32, (C, length), 0)
        allowed = key_place < query_place
        mixed = []
        for h in range(heads):
            part = slice(h * HEAD_DIM, (h + 1) * HEAD_DIM)
            vpart = slice(aw + h * HEAD_DIM, aw + (h + 1) * HEAD_DIM)
            s = dot_t(query_norm[h], kv[:, part]) * HEAD_DIM ** (-0.5) + offset[h]
            soft = jnp.log1p(jnp.exp(-jnp.abs(s)))
            rise = jnp.minimum(s, 0.0) - soft
            fail = jnp.where(allowed, jnp.minimum(-s, 0.0) - soft, 0.0)
            high, mid, low = split3(fail)
            sums = [
                jnp.sum(fail[:, d * C : (d + 1) * C], axis=1, keepdims=True) for d in range(E)
            ]
            afters = []
            for d in range(E):
                b = slice(d * C, (d + 1) * C)
                after = dot(high[:, b], later) + dot(mid[:, b], later) + dot(low[:, b], later)
                for o in range(E):
                    if o != d:
                        later_block = (column(o)[0] > column(d)[0]).astype(F32)
                        after = after + sums[o] * later_block
                afters.append(after)
            exponent = rise + jnp.concatenate(afters, axis=1)
            weights = jnp.where(allowed, jnp.exp(exponent), 0.0).astype(BF16)
            mixed.append(dot(weights, kv[:, vpart]))
        mixed = jnp.concatenate(mixed, axis=1).astype(BF16).astype(F32)
        rows = C // (2 * Z)
        for i in range(Z):
            for k in range(2):
                hm[i, k] = mixed[(2 * i + k) * rows : (2 * i + k + 1) * rows]

    hm_copy = rcopy(hm.at[:, 1 - core], hmo, hm_sem.at[0], hm_sem.at[1], partner)

    def mixer_terms():
        with jax.named_scope("w_mixer"):
         local[3].wait()
         swaps[3].wait_recv()
         hm_copy.wait_recv()
        rows = C // (2 * Z)
        mine = jnp.concatenate([hm[i, core] for i in range(Z)], axis=0).astype(BF16)
        other = jnp.concatenate([hmo[i] for i in range(Z)], axis=0).astype(BF16)
        terms = dot(mine, wm[0]) + dot(other, wm[1])
        for i in range(Z):
            ms[i] = terms[i * rows : (i + 1) * rows].astype(BF16)

    def expert(l):
        with jax.named_scope("w_plane_b"):
         rest(ob.at[l], xbs.at[l], pb_send.at[l], pb_recv.at[l]).wait_recv()
        hidden = []
        for i in range(2):
            g = dot_t(xa[l], wg[i, :, :A]) + dot_t(xbs[l], wg[i, :, A:])
            u = dot_t(xa[l], wu[i, :, :A]) + dot_t(xbs[l], wu[i, :, A:])
            hidden.append((g / (1.0 + jnp.exp(-g)) * u).astype(BF16))
        tile = 128 if A % 256 else 256
        for start in range(A, wide, tile):
            c = slice(start, start + tile)
            y = (dot(hidden[0], wd[0, :, c]) + dot(hidden[1], wd[1, :, c])).astype(BF16)
            pb[l, :, start - A : start - A + tile] = y
        for start in range(0, A, tile):
            c = slice(start, start + tile)
            y = (dot(hidden[0], wd[0, :, c]) + dot(hidden[1], wd[1, :, c])).astype(BF16)
            pa[l, :, c] = y

    def send_home(l):
        for d in range(1, E):
            plane(pb.at[l], qb.at[l], rb_send.at[l], rb_recv.at[l], d).start()
        qb[l, :cap] = pb[l, :cap]

    def ret_a(l, j, buf, recv, dev):
        s = pl.ds(j * R, R)
        return rcopy(pa.at[l, s], buf.at[l, s], za_send.at[l, j], recv.at[l, j], dev)

    def ret_b(l, j, buf, recv, dev):
        s = pl.ds(j * TR, TR)
        return rcopy(mb.at[l, s], buf.at[l, s], zb_send.at[l, j], recv.at[l, j], dev)

    def ret_m(l, buf, recv, dev):
        return rcopy(ms.at[l], buf.at[l], zm_send.at[l], recv.at[l], dev)

    def mix(l, s):
        return dot(wh[l, s], qb[l]) + dot(wl[l, s], qb[l])

    def returns_a(l, incoming, side):
        buf, recv, dev = ((ral, za_low, above), (rah, za_high, below))[side]
        for j in range(A_CHUNKS):
            s = pl.ds(j * R, R)

            @pl.when(incoming)
            def _():
                with jax.named_scope("w_ret_a"):
                    ret_a(l, j, buf, recv, dev).wait_recv()
                pa[l, s] = (pa[l, s].astype(F32) + buf[l, s].astype(F32)).astype(BF16)

            ret_a(l, j, buf, recv, dev).start()

    def returns_m(l, incoming, side):
        buf, recv, dev = ((rml, zm_low, above), (rmh, zm_high, below))[side]

        @pl.when(incoming)
        def _():
            ret_m(l, buf, recv, dev).wait_recv()
            ms[l] = (ms[l].astype(F32) + buf[l].astype(F32)).astype(BF16)

        ret_m(l, buf, recv, dev).start()

    def returns_b(l, incoming, side):
        buf, recv, dev = ((rbl, zb_low, above), (rbh, zb_high, below))[side]
        with jax.named_scope("w_ret_plane"):
            rest(pb.at[l], qb.at[l], rb_send.at[l], rb_recv.at[l]).wait_recv()
        for j in range(B_BACK):
            s = pl.ds(j * TR, TR)
            acc[...] = mix(l, s)

            @pl.when(incoming)
            def _():
                with jax.named_scope("w_ret_b"):
                    ret_b(l, j, buf, recv, dev).wait_recv()
                acc[...] = acc[...] + buf[l, s].astype(F32)

            mb[l, s] = acc[...].astype(BF16)
            ret_b(l, j, buf, recv, dev).start()

    def on_targets(t, work):
        target = t - z

        @pl.when(jnp.logical_and(target > z, target < Z))
        def _():
            work(target, has_low, 0)

        other = 2 * (Z - 1) - t - z

        @pl.when(jnp.logical_and(other >= 0, other < z))
        def _():
            work(other, has_high, 1)

    def levels_of(t, work):
        low = (z - t >= 0).astype(jnp.int32)
        high = jnp.logical_and(z + t < Z, t > 0).astype(jnp.int32)

        def side(i, carry):
            work(z + (2 * i - 1) * t)
            return carry

        lax.fori_loop(1 - low, 1 + high, side, 0)

    with jax.named_scope("w_weights"):
        for copy in local[:3]:
            copy.wait()
        for swap in swaps[:3]:
            swap.wait_recv()

    def tail_m(t, carry):
        on_targets(t, returns_m)
        return carry

    at_end = jnp.logical_or(z == 0, z == Z - 1)

    def slot_step(t, carry):
        with jax.named_scope("expert"):
            levels_of(t, expert)

        with jax.named_scope("ret_a"):
            on_targets(t, returns_a)

        @pl.when(jnp.logical_and(t > 0, t < Z - 1))
        def _():
            on_sides(t + 1, arrive_b)

        @pl.when(t > 0)
        def _():
            levels_of(t, send_home)

        @pl.when(t == Z - 1)
        def _():
            send_home(z)

        with jax.named_scope("ret_b"):
            on_targets(t - 1, returns_b)

        @pl.when(t == 1)
        def _():
            with jax.named_scope("attention"):
                attention()
            hm_copy.start()

        @pl.when(t < Z - 1)
        def _():
            on_sides(t + 1, arrive_a)

        @pl.when(t == 1)
        def _():
            with jax.named_scope("mixer"):
                mixer_terms()

            @pl.when(at_end)
            def _():
                lax.fori_loop(1, 2 * Z - 1, tail_m, 0)

        return carry

    lax.fori_loop(0, Z, slot_step, 0)

    @pl.when(jnp.logical_not(at_end))
    def _():
        with jax.named_scope("tail_m"):
            lax.fori_loop(1, 2 * Z - 1, tail_m, 0)

    def tail_a(t, carry):
        with jax.named_scope("tail_a"):
            on_targets(t, returns_a)
        return carry

    def tail_b(t, carry):
        with jax.named_scope("tail_b"):
            on_targets(t, returns_b)
        return carry

    lax.fori_loop(Z, 2 * Z - 1, tail_a, 0)
    lax.fori_loop(Z - 1, 2 * Z - 1, tail_b, 0)

    for j in range(A_CHUNKS):
        s = pl.ds(j * R, R)

        @pl.when(has_low)
        def _():
            with jax.named_scope("f_a_low"):
             ret_a(z, j, ral, za_low, above).wait_recv()
            pa[z, s] = (pa[z, s].astype(F32) + ral[z, s].astype(F32)).astype(BF16)

        @pl.when(has_high)
        def _():
            with jax.named_scope("f_a_high"):
             ret_a(z, j, rah, za_high, below).wait_recv()
            pa[z, s] = (pa[z, s].astype(F32) + rah[z, s].astype(F32)).astype(BF16)

        fa[s] = pa[z, s]
        if j == 0:
            qa[:cap] = pa[z, :cap]
        for d in range(max(1, j * R // cap), (j + 1) * R // cap):
            plane(fa, qa, ra_send, ra_recv, d).start()

    total = ms[z].astype(F32)
    att_out[...] = total.astype(BF16)

    @pl.when(has_low)
    def _():
        with jax.named_scope("f_m"):
            ret_m(z, rml, zm_low, above).wait_recv()
        att_out[...] = (att_out[...].astype(F32) + rml[z].astype(F32)).astype(BF16)

    @pl.when(has_high)
    def _():
        ret_m(z, rmh, zm_high, below).wait_recv()
        att_out[...] = (att_out[...].astype(F32) + rmh[z].astype(F32)).astype(BF16)

    rest(pb.at[z], qb.at[z], rb_send.at[z], rb_recv.at[z]).wait_recv()
    for j in range(B_BACK):
        s = pl.ds(j * TR, TR)
        acc[...] = mix(z, s)

        @pl.when(has_low)
        def _():
            with jax.named_scope("f_b_low"):
             ret_b(z, j, rbl, zb_low, above).wait_recv()
            acc[...] = acc[...] + rbl[z, s].astype(F32)

        @pl.when(has_high)
        def _():
            with jax.named_scope("f_b_high"):
             ret_b(z, j, rbh, zb_high, below).wait_recv()
            acc[...] = acc[...] + rbh[z, s].astype(F32)

        exp_out[s, A:] = acc[...].astype(BF16)

    with jax.named_scope("f_plane_a"):
     rest(fa, qa, ra_send, ra_recv).wait_recv()
    exp_out[:, :A] = (dot(wh[z], qa[...]) + dot(wl[z], qa[...])).astype(BF16)

    rest(oa, xa.at[z], pa_send, pa_recv).wait_send()
    rest(fa, qa, ra_send, ra_recv).wait_send()
    hm_copy.wait_send()
    for swap in swaps:
        swap.wait_send()
    for d in range(1, E):
        kv_copy(d).wait_send()

    def drain(l, carry):
        rest(ob.at[l], xbs.at[l], pb_send.at[l], pb_recv.at[l]).wait_send()
        rest(pb.at[l], qb.at[l], rb_send.at[l], rb_recv.at[l]).wait_send()

        @pl.when(jnp.logical_and(l <= z, has_high))
        def _():
            for j in range(B_CHUNKS):
                fwd_b(l, j, fb_up, above).wait_send()
            for j in range(A_CHUNKS):
                fwd_a(l, j, fa_up, above).wait_send()

        @pl.when(jnp.logical_and(l >= z, has_low))
        def _():
            for j in range(B_CHUNKS):
                fwd_b(l, j, fb_dn, below).wait_send()
            for j in range(A_CHUNKS):
                fwd_a(l, j, fa_dn, below).wait_send()

        @pl.when(l != z)
        def _():
            for j in range(A_CHUNKS):
                ret_a(l, j, ral, za_low, above).wait_send()
            for j in range(B_BACK):
                ret_b(l, j, rbl, zb_low, above).wait_send()
            ret_m(l, rml, zm_low, above).wait_send()

        return carry

    lax.fori_loop(0, Z, drain, 0)


def layer(
    query, key, value, query_gain, key_gain, offset, mixer, tokens, expert_gain, routes, scores,
    gate, up, down,
):
    E = lax.axis_size("ep")
    Z = lax.axis_size("tp") // 2
    C, D = tokens.shape
    H = gate.shape[2]
    aw = key.shape[1]
    A = D * EARLY_SHARE // 256
    A -= A % 128
    B = D - A
    slots = TOP_K * C
    rows = C // (2 * Z)
    dma = lambda *shape: pltpu.SemaphoreType.DMA(shape)
    vmem = pl.BlockSpec(memory_space=pltpu.VMEM)
    smem = pl.BlockSpec(memory_space=pltpu.SMEM)
    hbm = pl.BlockSpec(memory_space=pl.ANY)
    kernel = functools.partial(body, E, Z, C, D, A)
    NA, NB = A_CHUNKS, B_CHUNKS
    results = pl.pallas_call(
        kernel,
        name="step",
        out_shape=(
            jax.ShapeDtypeStruct((rows, D), BF16),
            jax.ShapeDtypeStruct((C, D), BF16),
        ),
        in_specs=[vmem, vmem, vmem, vmem, vmem, smem, hbm, vmem, vmem, vmem, vmem, hbm, hbm, hbm],
        out_specs=(vmem, vmem),
        scratch_shapes=[
            pltpu.VMEM((2, H, D), BF16),
            pltpu.VMEM((2, H, D), BF16),
            pltpu.VMEM((2, H, D), BF16),
            pltpu.VMEM((2, aw, D), BF16),
            pltpu.VMEM((C, D), BF16),
            pltpu.VMEM((Z, C, B + TAGS), BF16),
            pltpu.VMEM((Z, slots, A), BF16),
            pltpu.VMEM((Z, slots, B), BF16),
            pltpu.VMEM((slots, A), BF16),
            pltpu.VMEM((Z, slots, B), BF16),
            pltpu.VMEM((Z, slots, A), BF16),
            pltpu.VMEM((Z, slots, B), BF16),
            pltpu.VMEM((Z, slots, B), BF16),
            pltpu.VMEM((slots, A), BF16),
            pltpu.VMEM((Z, C, slots), BF16),
            pltpu.VMEM((Z, C, slots), BF16),
            pltpu.VMEM((Z, slots, A), BF16),
            pltpu.VMEM((Z, slots, A), BF16),
            pltpu.VMEM((Z, C, B), BF16),
            pltpu.VMEM((Z, C, B), BF16),
            pltpu.VMEM((Z, C, B), BF16),
            pltpu.VMEM((slots, A), BF16),
            pltpu.VMEM((C // B_BACK, B), F32),
            pltpu.VMEM((E * C, 2 * aw), BF16),
            pltpu.VMEM((Z, 2, rows, aw), F32),
            pltpu.VMEM((Z, rows, aw), F32),
            pltpu.VMEM((Z, rows, D), BF16),
            pltpu.VMEM((Z, rows, D), BF16),
            pltpu.VMEM((Z, rows, D), BF16),
            dma(4), dma(4), dma(4), dma(2),
            pltpu.SemaphoreType.DMA, pltpu.SemaphoreType.DMA,
            dma(E), dma(E),
            dma(Z), dma(Z),
            dma(Z), dma(Z),
            pltpu.SemaphoreType.DMA, pltpu.SemaphoreType.DMA,
            dma(Z, NB), dma(Z, NB), dma(Z, NB),
            dma(Z, NA), dma(Z, NA), dma(Z, NA),
            dma(Z, NA), dma(Z, NA), dma(Z, NA),
            dma(Z, B_BACK), dma(Z, B_BACK), dma(Z, B_BACK),
            dma(Z), dma(Z), dma(Z),
        ],
        compiler_params=pltpu.CompilerParams(
            collective_id=0, has_side_effects=True, vmem_limit_bytes=62 * 1024 * 1024
        ),
    )(
        query, key, value, query_gain[None], key_gain[None], offset, mixer, tokens,
        expert_gain[None], routes.T, scores.T, gate[0].T, up[0].T, down[0],
    )
    return pl.pallas_call(
        hand_over,
        name="hand_over",
        out_shape=(
            jax.ShapeDtypeStruct((rows, D), BF16),
            jax.ShapeDtypeStruct((C, D), BF16),
        ),
        in_specs=[vmem, vmem],
        out_specs=(hbm, hbm),
        scratch_shapes=[dma(2)],
    )(*results)


def hand_over(att_in, exp_in, att_out, exp_out, sems):
    first = pltpu.make_async_copy(att_in, att_out, sems.at[0])
    second = pltpu.make_async_copy(exp_in, exp_out, sems.at[1])
    second.start()
    first.start()
    second.wait()
    first.wait()


def solution(mesh):
    in_specs = (
        P("ep", "tp"),
        P("ep", "tp"),
        P("ep", "tp"),
        P(),
        P(),
        P("tp"),
        P("tp", None),
        P(("ep", "tp"), None),
        P(),
        P(("ep", "tp"), None),
        P(("ep", "tp"), None),
        P("ep", None, "tp"),
        P("ep", None, "tp"),
        P("ep", "tp", None),
    )
    out_specs = (P(("ep", "tp"), None), P(("ep", "tp"), None))
    return jax.shard_map(layer, mesh=mesh, in_specs=in_specs, out_specs=out_specs, check_vma=False)
```

```python
import functools

import jax
import jax.numpy as jnp
from jax import lax
from jax.experimental import pallas as pl
from jax.experimental.pallas import tpu as pltpu
from jax.sharding import PartitionSpec as P

HEAD_DIM = 64
TOP_K = 2
EPS = 1e-06
TAGS = 8
MESH = pl.DeviceIdType.MESH
F32, BF16 = jnp.float32, jnp.bfloat16

EARLY_SHARE = 96
A_CHUNKS = 4
A_BACK = 4
B_CHUNKS = 2
B_BACK = 8


def dot(a, b):
    return jnp.dot(a, b, preferred_element_type=F32)


def dot_t(a, b):
    return lax.dot_general(a, b, (((1,), (1,)), ((), ())), preferred_element_type=F32)


def split3(x):
    high = x.astype(BF16)
    rest = x - high.astype(F32)
    mid = rest.astype(BF16)
    low = (rest - mid.astype(F32)).astype(BF16)
    return high, mid, low


def rcopy(src, dst, send, recv, dev):
    return pltpu.make_async_remote_copy(
        src_ref=src, dst_ref=dst, send_sem=send, recv_sem=recv, device_id=dev, device_id_type=MESH
    )


def norm_heads(ref, gain):
    out = []
    for start in range(0, ref.shape[1], HEAD_DIM):
        x = ref[:, start : start + HEAD_DIM].astype(F32)
        x = x * lax.rsqrt(jnp.mean(x * x, axis=1, keepdims=True) + EPS)
        out.append((x * gain).astype(BF16))
    return out


def body(
    experts, levels, count, wide, early,
    query_in, key_in, value_in, query_gain_in, key_gain_in, offset_in, mixer, tokens_in,
    expert_gain_in, routes_in, scores_in, gate, up, down,
    att_out, exp_out,
    query, key, value, query_gain, key_gain, offset, tokens, expert_gain, routes, scores, in_sem,
    wg, wu, wd, wm, normed, tg, xb, xa, xbs, oa, ob, pa, pb, qb, qa, wh, wl,
    ral, rah, mb, rbl, rbh, fa, acc, kv, hm, hmo, ms, rml, rmh,
    lw_sem, pw_send, pw_recv, hm_sem,
    pa_send, pa_recv, kv_send, kv_recv, pb_send, pb_recv, rb_send, rb_recv, ra_send, ra_recv,
    ft_up, ft_dn, ft_recv, fb_up, fb_dn, fb_recv, fa_up, fa_dn, fa_recv,
    za_send, za_low, za_high, zb_send, zb_low, zb_high, zm_send, zm_low, zm_high,
):
    E, Z, C = experts, levels, count
    A, B = early, wide - early
    slots = TOP_K * C
    cap = slots // E
    R = slots // A_CHUNKS
    TB = C // B_CHUNKS
    TR = C // B_BACK
    RR = slots // A_BACK
    ep = lax.axis_index("ep")
    tp = lax.axis_index("tp")
    z = tp // 2
    core = tp % 2
    partner = (ep, tp + 1 - 2 * core)
    above = (ep, tp + 2)
    below = (ep, tp - 2)
    has_low = z > 0
    has_high = z < Z - 1

    def column(d):
        index, bit = ep, 1
        while bit < E:
            if d & bit:
                index = index + bit * (1 - 2 * ((ep // bit) % 2))
            bit *= 2
        return (index, tp)

    barrier = pltpu.get_barrier_semaphore()
    for d in range(1, E):
        pl.semaphore_signal(barrier, inc=1, device_id=column(d), device_id_type=MESH)
    pl.semaphore_signal(barrier, inc=1, device_id=partner, device_id_type=MESH)

    @pl.when(has_low)
    def _():
        pl.semaphore_signal(barrier, inc=1, device_id=below, device_id_type=MESH)

    @pl.when(has_high)
    def _():
        pl.semaphore_signal(barrier, inc=1, device_id=above, device_id_type=MESH)

    arrays = (
        (tokens_in, tokens), (expert_gain_in, expert_gain), (routes_in, routes),
        (scores_in, scores), (key_in, key), (value_in, value), (key_gain_in, key_gain),
        (query_in, query), (query_gain_in, query_gain), (offset_in, offset),
    )
    loads = [pltpu.make_async_copy(src, dst, in_sem.at[i]) for i, (src, dst) in enumerate(arrays)]
    for load in loads:
        load.start()
    local = [
        pltpu.make_async_copy(src, dst.at[0], lw_sem.at[i])
        for i, (src, dst) in enumerate(((gate, wg), (up, wu), (down, wd), (mixer, wm)))
    ]
    for copy in local:
        copy.start()
    for load in loads[:4]:
        load.wait()

    x = tokens[...].astype(F32)
    x = x * lax.rsqrt(jnp.mean(x * x, axis=1, keepdims=True) + EPS) * expert_gain[...]
    normed[...] = x.astype(BF16)
    route = routes[...].astype(F32)
    s0, s1 = scores[0:1], scores[1:2]
    w0 = 1.0 / (1.0 + jnp.exp(s1 - s0))
    w1 = 1.0 / (1.0 + jnp.exp(s0 - s1))
    line = lax.broadcasted_iota(jnp.int32, (TAGS, C), 0)
    label = jnp.zeros((TAGS, C), F32)
    for i, piece in enumerate((route[0:1], route[1:2], w0, w1)):
        label = jnp.where(line == i, piece, label)
    tg[z] = label
    xb[z] = normed[:, A:]

    def fwd_t(l, sems, dev):
        return rcopy(tg.at[l], tg.at[l], sems.at[l], ft_recv.at[l], dev)

    def fwd_b(l, j, sems, dev):
        s = pl.ds(j * TB, TB)
        return rcopy(xb.at[l, s], xb.at[l, s], sems.at[l], fb_recv.at[l, j], dev)

    def fwd_a(l, j, sems, dev):
        s = pl.ds(j * R, R)
        return rcopy(xa.at[l, s], xa.at[l, s], sems.at[l], fa_recv.at[l, j], dev)

    def both_ways(make, chunks, up_sems, dn_sems):
        for j in range(chunks):

            @pl.when(has_high)
            def _():
                make(z, j, up_sems, above).start()

            @pl.when(has_low)
            def _():
                make(z, j, dn_sems, below).start()

    row = lax.broadcasted_iota(jnp.int32, (C, C), 0)
    col = lax.broadcasted_iota(jnp.int32, (C, C), 1)
    before = (col < row).astype(F32).astype(BF16)
    later = (row > col).astype(F32).astype(BF16)
    slot = lax.broadcasted_iota(jnp.int32, (C, slots), 1)
    shift = cap.bit_length() - 1
    slot_expert = jnp.bitwise_xor(lax.shift_right_logical(slot, shift), ep).astype(F32)
    slot_rank = jnp.bitwise_and(slot, cap - 1).astype(F32)

    def selection(l):
        t = jnp.concatenate([tg[l], jnp.zeros((C - TAGS, C), F32)], axis=0).T
        m0 = t[:, 0:1] == slot_expert
        m1 = t[:, 1:2] == slot_expert
        member = jnp.where(jnp.logical_or(m0, m1), 1.0, 0.0)
        rank = dot(before, member.astype(BF16))
        chosen = jnp.where(rank == slot_rank, member, 0.0)
        weight = chosen * jnp.where(m0, t[:, 2:3], t[:, 3:4])
        high = weight.astype(BF16)
        wh[l] = high
        wl[l] = (weight - high.astype(F32)).astype(BF16)
        return chosen.T.astype(BF16)

    def plane(src, dst, send, recv, d):
        s = pl.ds(d * cap, cap)
        return rcopy(src.at[s], dst.at[s], send, recv, column(d))

    def rest(src, dst, send, recv):
        s = pl.ds(cap, slots - cap)
        return rcopy(src.at[s], dst.at[s], send, recv, column(1))

    def dispatch_b(l, chosen):
        out = dot(chosen, xb[l]).astype(BF16)
        xbs[l, :cap] = out[:cap]
        ob[l, cap:] = out[cap:]
        for d in range(1, E):
            plane(ob.at[l], xbs.at[l], pb_send.at[l], pb_recv.at[l], d).start()

    chosen = selection(z)
    out = dot(chosen, normed[:, :A]).astype(BF16)
    xa[z, :cap] = out[:cap]
    oa[cap:] = out[cap:]
    with jax.named_scope("barrier"):
     pl.semaphore_wait(barrier, E + has_low.astype(jnp.int32) + has_high.astype(jnp.int32))

    both_ways(lambda l, j, sems, dev: fwd_t(l, sems, dev), 1, ft_up, ft_dn)
    both_ways(fwd_b, B_CHUNKS, fb_up, fb_dn)
    for d in range(1, E):
        plane(oa, xa.at[z], pa_send, pa_recv.at[d], d).start()

    swaps = [
        rcopy(src, dst.at[1], pw_send.at[i], pw_recv.at[i], partner)
        for i, (src, dst) in enumerate(((gate, wg), (up, wu), (down, wd), (mixer, wm)))
    ]
    for swap in swaps:
        swap.start()

    dispatch_b(z, chosen)

    for j in range(A_CHUNKS):
        with jax.named_scope("w_own_a"):
            for d in range(max(1, j * R // cap), (j + 1) * R // cap):
                plane(oa, xa.at[z], pa_send, pa_recv.at[d], d).wait_recv()

        @pl.when(has_high)
        def _():
            fwd_a(z, j, fa_up, above).start()

        @pl.when(has_low)
        def _():
            fwd_a(z, j, fa_dn, below).start()


    def on_sides(t, work):
        @pl.when(z - t >= 0)
        def _():
            work(z - t, has_high, 0)

        @pl.when(z + t < Z)
        def _():
            work(z + t, has_low, 1)

    def arrive_b(l, onward, side):
        sems, dev = ((fb_up, above), (fb_dn, below))[side]
        tags = fwd_t(l, (ft_up, ft_dn)[side], dev)
        tags.wait_recv()

        @pl.when(onward)
        def _():
            tags.start()

        for j in range(B_CHUNKS):
            with jax.named_scope("w_fwd_b"):
                fwd_b(l, j, sems, dev).wait_recv()

            @pl.when(onward)
            def _():
                fwd_b(l, j, sems, dev).start()

        with jax.named_scope("dispatch"):
            dispatch_b(l, selection(l))

    def arrive_a(l, onward, side):
        sems, dev = ((fa_up, above), (fa_dn, below))[side]
        for j in range(A_CHUNKS):
            with jax.named_scope("w_fwd_a"):
                fwd_a(l, j, sems, dev).wait_recv()

            @pl.when(onward)
            def _():
                fwd_a(l, j, sems, dev).start()

    on_sides(1, arrive_b)

    heads = key.shape[1] // HEAD_DIM
    aw = key.shape[1]
    for load in loads[4:7]:
        load.wait()
    kv[:C, :aw] = jnp.concatenate(norm_heads(key, key_gain[...]), axis=1)
    kv[:C, aw:] = value[...]

    def kv_copy(d):
        return rcopy(kv.at[pl.ds(0, C)], kv.at[pl.ds(d * C, C)], kv_send.at[d], kv_recv.at[d], column(d))

    for d in range(1, E):
        kv_copy(d).start()

    def attention():
        with jax.named_scope("w_kv"):
         for d in range(1, E):
            kv_copy(d).wait_recv()
        length = E * C
        for load in loads[7:]:
            load.wait()
        query_norm = norm_heads(query, query_gain[...])
        lane = lax.broadcasted_iota(jnp.int32, (C, length), 1)
        bits = C.bit_length() - 1
        owner = jnp.bitwise_xor(lax.shift_right_logical(lane, bits), ep)
        key_place = owner * C + jnp.bitwise_and(lane, C - 1)
        query_place = ep * C + lax.broadcasted_iota(jnp.int32, (C, length), 0)
        allowed = key_place < query_place
        mixed = []
        for h in range(heads):
            part = slice(h * HEAD_DIM, (h + 1) * HEAD_DIM)
            vpart = slice(aw + h * HEAD_DIM, aw + (h + 1) * HEAD_DIM)
            s = dot_t(query_norm[h], kv[:, part]) * HEAD_DIM ** (-0.5) + offset[:, h : h + 1]
            soft = jnp.log1p(jnp.exp(-jnp.abs(s)))
            rise = jnp.minimum(s, 0.0) - soft
            fail = jnp.where(allowed, jnp.minimum(-s, 0.0) - soft, 0.0)
            high, mid, low = split3(fail)
            sums = [
                jnp.sum(fail[:, d * C : (d + 1) * C], axis=1, keepdims=True) for d in range(E)
            ]
            afters = []
            for d in range(E):
                b = slice(d * C, (d + 1) * C)
                after = dot(high[:, b], later) + dot(mid[:, b], later) + dot(low[:, b], later)
                for o in range(E):
                    if o != d:
                        later_block = (column(o)[0] > column(d)[0]).astype(F32)
                        after = after + sums[o] * later_block
                afters.append(after)
            exponent = rise + jnp.concatenate(afters, axis=1)
            weights = jnp.where(allowed, jnp.exp(exponent), 0.0).astype(BF16)
            mixed.append(dot(weights, kv[:, vpart]))
        mixed = jnp.concatenate(mixed, axis=1).astype(BF16).astype(F32)
        rows = C // (2 * Z)
        for i in range(Z):
            for k in range(2):
                hm[i, k] = mixed[(2 * i + k) * rows : (2 * i + k + 1) * rows]

    hm_copy = rcopy(hm.at[:, 1 - core], hmo, hm_sem.at[0], hm_sem.at[1], partner)

    def mixer_terms():
        with jax.named_scope("w_mixer"):
         local[3].wait()
         swaps[3].wait_recv()
         hm_copy.wait_recv()
        rows = C // (2 * Z)
        mine = jnp.concatenate([hm[i, core] for i in range(Z)], axis=0).astype(BF16)
        other = jnp.concatenate([hmo[i] for i in range(Z)], axis=0).astype(BF16)
        terms = dot(mine, wm[0]) + dot(other, wm[1])
        for i in range(Z):
            ms[i] = terms[i * rows : (i + 1) * rows].astype(BF16)

    def expert(l):
        with jax.named_scope("w_plane_b"):
         rest(ob.at[l], xbs.at[l], pb_send.at[l], pb_recv.at[l]).wait_recv()
        hidden = []
        for i in range(2):
            g = dot_t(xa[l], wg[i, :, :A]) + dot_t(xbs[l], wg[i, :, A:])
            u = dot_t(xa[l], wu[i, :, :A]) + dot_t(xbs[l], wu[i, :, A:])
            hidden.append((g / (1.0 + jnp.exp(-g)) * u).astype(BF16))
        tile = 128 if A % 256 else 256
        for start in range(A, wide, tile):
            c = slice(start, start + tile)
            y = (dot(hidden[0], wd[0, :, c]) + dot(hidden[1], wd[1, :, c])).astype(BF16)
            pb[l, :, start - A : start - A + tile] = y
        for start in range(0, A, tile):
            c = slice(start, start + tile)
            y = (dot(hidden[0], wd[0, :, c]) + dot(hidden[1], wd[1, :, c])).astype(BF16)
            pa[l, :, c] = y

    def send_home(l):
        for d in range(1, E):
            plane(pb.at[l], qb.at[l], rb_send.at[l], rb_recv.at[l], d).start()
        qb[l, :cap] = pb[l, :cap]

    def ret_a(l, j, buf, recv, dev):
        s = pl.ds(j * RR, RR)
        return rcopy(pa.at[l, s], buf.at[l, s], za_send.at[l], recv.at[l, j], dev)

    def ret_b(l, j, buf, recv, dev):
        s = pl.ds(j * TR, TR)
        return rcopy(mb.at[l, s], buf.at[l, s], zb_send.at[l], recv.at[l, j], dev)

    def ret_m(l, buf, recv, dev):
        return rcopy(ms.at[l], buf.at[l], zm_send.at[l], recv.at[l], dev)

    def mix(l, rows):
        return dot(wh[l], rows) + dot(wl[l], rows)

    def returns_a(l, incoming, side):
        buf, recv, dev = ((ral, za_low, above), (rah, za_high, below))[side]
        for j in range(A_BACK):
            s = pl.ds(j * RR, RR)

            @pl.when(incoming)
            def _():
                with jax.named_scope("w_ret_a"):
                    ret_a(l, j, buf, recv, dev).wait_recv()
                pa[l, s] = (pa[l, s].astype(F32) + buf[l, s].astype(F32)).astype(BF16)

            ret_a(l, j, buf, recv, dev).start()

    def returns_m(l, incoming, side):
        buf, recv, dev = ((rml, zm_low, above), (rmh, zm_high, below))[side]

        @pl.when(incoming)
        def _():
            ret_m(l, buf, recv, dev).wait_recv()
            ms[l] = (ms[l].astype(F32) + buf[l].astype(F32)).astype(BF16)

        ret_m(l, buf, recv, dev).start()

    def returns_b(l, incoming, side):
        buf, recv, dev = ((rbl, zb_low, above), (rbh, zb_high, below))[side]
        with jax.named_scope("w_ret_plane"):
            rest(pb.at[l], qb.at[l], rb_send.at[l], rb_recv.at[l]).wait_recv()
        acc[...] = mix(l, qb[l])
        for j in range(B_BACK):
            s = pl.ds(j * TR, TR)

            @pl.when(incoming)
            def _():
                with jax.named_scope("w_ret_b"):
                    ret_b(l, j, buf, recv, dev).wait_recv()
                acc[s] = acc[s] + buf[l, s].astype(F32)

            mb[l, s] = acc[s].astype(BF16)
            ret_b(l, j, buf, recv, dev).start()

    def on_targets(t, work):
        target = t - z

        @pl.when(jnp.logical_and(target > z, target < Z))
        def _():
            work(target, has_low, 0)

        other = 2 * (Z - 1) - t - z

        @pl.when(jnp.logical_and(other >= 0, other < z))
        def _():
            work(other, has_high, 1)

    def levels_of(t, work):
        low = (z - t >= 0).astype(jnp.int32)
        high = jnp.logical_and(z + t < Z, t > 0).astype(jnp.int32)

        def side(i, carry):
            work(z + (2 * i - 1) * t)
            return carry

        lax.fori_loop(1 - low, 1 + high, side, 0)

    with jax.named_scope("w_weights"):
        for copy in local[:3]:
            copy.wait()
        for swap in swaps[:3]:
            swap.wait_recv()

    def tail_m(t, carry):
        on_targets(t, returns_m)
        return carry

    at_end = jnp.logical_or(z == 0, z == Z - 1)

    def slot_step(t, carry):
        with jax.named_scope("expert"):
            levels_of(t, expert)

        with jax.named_scope("ret_a"):
            on_targets(t, returns_a)

        @pl.when(jnp.logical_and(t > 0, t < Z - 1))
        def _():
            on_sides(t + 1, arrive_b)

        @pl.when(t == Z - 1)
        def _():
            levels_of(t, send_home)

        @pl.when(jnp.logical_and(t == Z - 1, jnp.logical_not(at_end)))
        def _():
            send_home(z)

        with jax.named_scope("ret_b"):
            on_targets(t - 1, returns_b)

        @pl.when(t == 1)
        def _():
            with jax.named_scope("attention"):
                attention()
            hm_copy.start()

        @pl.when(t < Z - 1)
        def _():
            on_sides(t + 1, arrive_a)

        @pl.when(jnp.logical_and(t > 0, t < Z - 1))
        def _():
            levels_of(t, send_home)

        @pl.when(t == 1)
        def _():
            with jax.named_scope("mixer"):
                mixer_terms()

            @pl.when(at_end)
            def _():
                lax.fori_loop(1, 2 * Z - 1, tail_m, 0)

        return carry

    lax.fori_loop(0, Z, slot_step, 0)

    @pl.when(jnp.logical_not(at_end))
    def _():
        with jax.named_scope("tail_m"):
            lax.fori_loop(1, 2 * Z - 1, tail_m, 0)

    def tail_a(t, carry):
        with jax.named_scope("tail_a"):
            on_targets(t, returns_a)
        return carry

    def tail_b(t, carry):
        with jax.named_scope("tail_b"):
            on_targets(t, returns_b)
        return carry

    def own_a():
        for j in range(A_BACK):
            s = pl.ds(j * RR, RR)

            @pl.when(has_low)
            def _():
                with jax.named_scope("f_a_low"):
                 ret_a(z, j, ral, za_low, above).wait_recv()
                pa[z, s] = (pa[z, s].astype(F32) + ral[z, s].astype(F32)).astype(BF16)

            @pl.when(has_high)
            def _():
                with jax.named_scope("f_a_high"):
                 ret_a(z, j, rah, za_high, below).wait_recv()
                pa[z, s] = (pa[z, s].astype(F32) + rah[z, s].astype(F32)).astype(BF16)

            fa[s] = pa[z, s]
            if (j + 1) * RR == max(cap, RR):
                qa[:cap] = pa[z, :cap]
            for d in range(max(1, j * RR // cap), (j + 1) * RR // cap):
                plane(fa, qa, ra_send, ra_recv, d).start()

    def tail(t, carry):
        tail_a(t, carry)

        @pl.when(jnp.logical_and(t == 2 * Z - 2, jnp.logical_not(at_end)))
        def _():
            own_a()

        tail_b(t - 1, carry)
        return carry

    lax.fori_loop(Z, 2 * Z, tail, 0)

    @pl.when(at_end)
    def _():
        send_home(z)
        own_a()


    total = ms[z].astype(F32)
    att_out[...] = total.astype(BF16)

    @pl.when(has_low)
    def _():
        with jax.named_scope("f_m"):
            ret_m(z, rml, zm_low, above).wait_recv()
        att_out[...] = (att_out[...].astype(F32) + rml[z].astype(F32)).astype(BF16)

    @pl.when(has_high)
    def _():
        ret_m(z, rmh, zm_high, below).wait_recv()
        att_out[...] = (att_out[...].astype(F32) + rmh[z].astype(F32)).astype(BF16)

    rest(pb.at[z], qb.at[z], rb_send.at[z], rb_recv.at[z]).wait_recv()
    acc[...] = mix(z, qb[z])
    rest(oa, xa.at[z], pa_send, pa_recv.at[1]).wait_send()
    rest(fa, qa, ra_send, ra_recv).wait_send()
    hm_copy.wait_send()
    for swap in swaps:
        swap.wait_send()
    for d in range(1, E):
        kv_copy(d).wait_send()

    def drain(l, carry):
        rest(ob.at[l], xbs.at[l], pb_send.at[l], pb_recv.at[l]).wait_send()
        rest(pb.at[l], qb.at[l], rb_send.at[l], rb_recv.at[l]).wait_send()

        @pl.when(jnp.logical_and(l <= z, has_high))
        def _():
            fwd_t(l, ft_up, above).wait_send()
            rcopy(xb.at[l], xb.at[l], fb_up.at[l], fb_recv.at[l, 0], above).wait_send()
            rcopy(xa.at[l], xa.at[l], fa_up.at[l], fa_recv.at[l, 0], above).wait_send()

        @pl.when(jnp.logical_and(l >= z, has_low))
        def _():
            fwd_t(l, ft_dn, below).wait_send()
            rcopy(xb.at[l], xb.at[l], fb_dn.at[l], fb_recv.at[l, 0], below).wait_send()
            rcopy(xa.at[l], xa.at[l], fa_dn.at[l], fa_recv.at[l, 0], below).wait_send()

        @pl.when(l != z)
        def _():
            rcopy(pa.at[l], ral.at[l], za_send.at[l], za_low.at[l, 0], above).wait_send()
            rcopy(mb.at[l], rbl.at[l], zb_send.at[l], zb_low.at[l, 0], above).wait_send()
            ret_m(l, rml, zm_low, above).wait_send()

        return carry

    with jax.named_scope("drain"):
        lax.fori_loop(0, Z, drain, 0)

    for j in range(B_BACK):
        s = pl.ds(j * TR, TR)

        @pl.when(has_low)
        def _():
            with jax.named_scope("f_b_low"):
                ret_b(z, j, rbl, zb_low, above).wait_recv()
            acc[s] = acc[s] + rbl[z, s].astype(F32)

        @pl.when(has_high)
        def _():
            with jax.named_scope("f_b_high"):
                ret_b(z, j, rbh, zb_high, below).wait_recv()
            acc[s] = acc[s] + rbh[z, s].astype(F32)

        exp_out[s, A:] = acc[s].astype(BF16)

    with jax.named_scope("f_plane_a"):
        rest(fa, qa, ra_send, ra_recv).wait_recv()
    exp_out[:, :A] = mix(z, qa[...]).astype(BF16)

def layer(
    query, key, value, query_gain, key_gain, offset, mixer, tokens, expert_gain, routes, scores,
    gate, up, down,
):
    E = lax.axis_size("ep")
    Z = lax.axis_size("tp") // 2
    C, D = tokens.shape
    H = gate.shape[2]
    aw = key.shape[1]
    A = D * EARLY_SHARE // 256
    A -= A % 128
    B = D - A
    slots = TOP_K * C
    rows = C // (2 * Z)
    dma = lambda *shape: pltpu.SemaphoreType.DMA(shape)
    vmem = pl.BlockSpec(memory_space=pltpu.VMEM)
    hbm = pl.BlockSpec(memory_space=pl.ANY)
    kernel = functools.partial(body, E, Z, C, D, A)
    NA, NB = A_CHUNKS, B_CHUNKS
    return pl.pallas_call(
        kernel,
        name="step",
        out_shape=(pltpu.VMEM((rows, D), BF16), pltpu.VMEM((C, D), BF16)),
        in_specs=[hbm] * 14,
        out_specs=(vmem, vmem),
        scratch_shapes=[
            pltpu.VMEM((C, aw), BF16),
            pltpu.VMEM((C, aw), BF16),
            pltpu.VMEM((C, aw), BF16),
            pltpu.VMEM((1, HEAD_DIM), F32),
            pltpu.VMEM((1, HEAD_DIM), F32),
            pltpu.VMEM((1, aw // HEAD_DIM), F32),
            pltpu.VMEM((C, D), BF16),
            pltpu.VMEM((1, D), F32),
            pltpu.VMEM((TOP_K, C), jnp.int32),
            pltpu.VMEM((TOP_K, C), F32),
            dma(10),
            pltpu.VMEM((2, H, D), BF16),
            pltpu.VMEM((2, H, D), BF16),
            pltpu.VMEM((2, H, D), BF16),
            pltpu.VMEM((2, aw, D), BF16),
            pltpu.VMEM((C, D), BF16),
            pltpu.VMEM((Z, TAGS, C), F32),
            pltpu.VMEM((Z, C, B), BF16),
            pltpu.VMEM((Z, slots, A), BF16),
            pltpu.VMEM((Z, slots, B), BF16),
            pltpu.VMEM((slots, A), BF16),
            pltpu.VMEM((Z, slots, B), BF16),
            pltpu.VMEM((Z, slots, A), BF16),
            pltpu.VMEM((Z, slots, B), BF16),
            pltpu.VMEM((Z, slots, B), BF16),
            pltpu.VMEM((slots, A), BF16),
            pltpu.VMEM((Z, C, slots), BF16),
            pltpu.VMEM((Z, C, slots), BF16),
            pltpu.VMEM((Z, slots, A), BF16),
            pltpu.VMEM((Z, slots, A), BF16),
            pltpu.VMEM((Z, C, B), BF16),
            pltpu.VMEM((Z, C, B), BF16),
            pltpu.VMEM((Z, C, B), BF16),
            pltpu.VMEM((slots, A), BF16),
            pltpu.VMEM((C, B), F32),
            pltpu.VMEM((E * C, 2 * aw), BF16),
            pltpu.VMEM((Z, 2, rows, aw), F32),
            pltpu.VMEM((Z, rows, aw), F32),
            pltpu.VMEM((Z, rows, D), BF16),
            pltpu.VMEM((Z, rows, D), BF16),
            pltpu.VMEM((Z, rows, D), BF16),
            dma(4), dma(4), dma(4), dma(2),
            pltpu.SemaphoreType.DMA, dma(E),
            dma(E), dma(E),
            dma(Z), dma(Z),
            dma(Z), dma(Z),
            pltpu.SemaphoreType.DMA, pltpu.SemaphoreType.DMA,
            dma(Z), dma(Z), dma(Z),
            dma(Z), dma(Z), dma(Z, NB),
            dma(Z), dma(Z), dma(Z, NA),
            dma(Z), dma(Z, A_BACK), dma(Z, A_BACK),
            dma(Z), dma(Z, B_BACK), dma(Z, B_BACK),
            dma(Z), dma(Z), dma(Z),
        ],
        compiler_params=pltpu.CompilerParams(
            collective_id=0, has_side_effects=True, vmem_limit_bytes=62 * 1024 * 1024
        ),
    )(
        query, key, value, query_gain[None], key_gain[None], offset[None], mixer, tokens,
        expert_gain[None], routes.T, scores.T, gate[0].T, up[0].T, down[0],
    )


def solution(mesh):
    in_specs = (
        P("ep", "tp"),
        P("ep", "tp"),
        P("ep", "tp"),
        P(),
        P(),
        P("tp"),
        P("tp", None),
        P(("ep", "tp"), None),
        P(),
        P(("ep", "tp"), None),
        P(("ep", "tp"), None),
        P("ep", None, "tp"),
        P("ep", None, "tp"),
        P("ep", "tp", None),
    )
    out_specs = (P(("ep", "tp"), None), P(("ep", "tp"), None))
    return jax.shard_map(layer, mesh=mesh, in_specs=in_specs, out_specs=out_specs, check_vma=False)
```
